32 devices in a mesh: sp: 8 (over z, y), tp: 4 (over x, core).
Axes of the slice: x: 2, y: 2, z: 4, core: 2. Of those that a mesh axis runs over, the one named last changes fastest.
Arguments:
- tokens: bfloat16 [8192, 2048], P('sp'), may hold values from -6 to 6
- norm_gain: bfloat16 [2048], replicated, may hold values from 0.099609375 to 1.8984375
- value_proj: bfloat16 [2048, 1024], P('sp', 'tp'), may hold values from -0.125 to 0.125
- glu_proj: bfloat16 [2048, 1024], P('sp', 'tp'), may hold values from -0.125 to 0.125
- recur_proj: bfloat16 [2048, 1024], P('sp', 'tp'), may hold values from -0.125 to 0.125
- branch_proj: bfloat16 [2048, 1024], P('sp', 'tp'), may hold values from -0.125 to 0.125
- channelwise_filter_taps: bfloat16 [31, 1024], P(None, 'tp'), may hold values from -1 to 1
- group_gain: bfloat16 [1024], P('tp'), may hold values from 0.099609375 to 1.8984375
- short_kernel: bfloat16 [4, 1024], P(None, 'tp'), may hold values from -3 to 3
- decay_map: bfloat16 [16, 64, 64], P('tp'), may hold values from -0.75 to 0.75
- entry_gate_matrix: bfloat16 [16, 64, 64], P('tp'), may hold values from -0.75 to 0.75
- rate_param: float32 [1024], P('tp'), may hold values from 4.5 to 15, as said below
- extra_decay: float32 [8192, 1024], P('sp', 'tp'), may hold values from -1 to 0, as said below
- conv_out: bfloat16 [1024, 2048], P('tp', 'sp'), may hold values from -0.125 to 0.125
- recur_out: bfloat16 [1024, 2048], P('tp', 'sp'), may hold values from -0.125 to 0.125
Outputs:
- mixed: bfloat16 [8192, 2048], P(('sp', 'tp'))
The draws below stay inside these ranges and needn't reach their ends.
Inputs may be any that keep to these rules, and one draw needn't show every extreme that they name: `rate_param`: a finite parameter of each channel. `extra_decay`: every entry is negative.
All inputs are finite; a program needn't handle non-finite values.
Results may differ from the reference program's by a relative error of at most 0.015.
Values may be sent and summed in bfloat16 or wider, within the bound.
No kernel may reach another device: no remote copies, remote signals or barrier semaphores. Data moves between devices by JAX's collectives and lax.ppermute only.
A program may use at most 64 MiB of HBM per device.

```python
import math
import jax
import jax.numpy as jnp
from jax import lax

D = 2048
CONV_CH = 1024
GROUP_CH = 64
LRU_CH = 1024
HEAD_CH = 64
KERNEL = 31
SHORT = 4
TOK_DEV = 1024
TOKENS = 8192
LRU_HEADS = 16


def draw_rate_param(key, part):
    heads = LRU_CH // HEAD_CH
    key_kind, key_slow, key_fast = jax.random.split(jax.random.fold_in(key, 11), 3)
    share = 0.5
    chooser = jax.random.uniform(key_kind, (heads,), jnp.float32) < share
    slow_kind = jnp.repeat(chooser, HEAD_CH)
    slow_rate = jnp.exp(jax.random.uniform(key_slow, (LRU_CH,), jnp.float32, math.log(0.15), math.log(0.6))) / (4.0 * TOKENS)
    fast_rate = 0.005 * jnp.exp(jax.random.uniform(key_fast, (LRU_CH,), jnp.float32, math.log(0.6), math.log(1.6)))
    rate = jnp.where(slow_kind, slow_rate, fast_rate)
    return -jnp.log(jnp.expm1(rate))


def draw_extra_decay(key, part):
    span = TOK_DEV // 4
    blocks = TOKENS // span
    heads = LRU_CH // HEAD_CH
    key_rate, key_spot, depth_random_key = jax.random.split(jax.random.fold_in(key, 23), 3)
    level = jnp.exp(jax.random.uniform(key_rate, (blocks, heads), jnp.float32, math.log(0.1), math.log(1.0))) / TOKENS
    blending_coefficient = jnp.repeat(jnp.repeat(level, span, axis=0), HEAD_CH, axis=1)
    spots_at = jax.random.randint(key_spot, (2,), 0, TOKENS)
    filter_extent = jnp.log(jax.random.uniform(depth_random_key, (2,), jnp.float32, 0.5, 0.8))
    agreement_tally = (jnp.arange(TOKENS)[:, None] == spots_at[None, :]).astype(jnp.float32)
    packet_clusters = jnp.sum(agreement_tally * filter_extent[None, :], axis=1)
    return -blending_coefficient + packet_clusters[:, None]


def steps_of(key, dims, cuts, smallest, high):
    def one(dim, parts):
        draws = jax.random.uniform(jax.random.fold_in(jax.random.fold_in(key, 6), dim), (parts,), jnp.float32, smallest / len(cuts), high / len(cuts))
        return jnp.repeat(jnp.exp(draws), dims[dim] // parts).reshape((-1,) + (1,) * (len(dims) - dim - 1))

    factor_of = one(*cuts[0])
    for cut in cuts[1:]:
        factor_of = factor_of * one(*cut)
    return factor_of


def noise(stream_key, shape, scale, most, pieces=(), held_as=jnp.bfloat16):
    entries = scale * jax.random.normal(stream_key, shape, jnp.float32)
    if pieces:
        entries = entries * steps_of(stream_key, shape, pieces, -0.22, 0.18)
    return jnp.clip(entries, -most, most).astype(held_as)


def setup_inputs(seed: int = 0) -> dict:
    keys = jax.random.split(jax.random.key(seed), 16)
    tokens = noise(keys[0], (TOKENS, D), 1.0, 6.0, ((0, 8),))
    norm_gain = jnp.clip(1.0 + 0.18 * jax.random.normal(keys[1], (D,), jnp.float32), 0.099609375, 1.8984375).astype(jnp.bfloat16)
    value_proj = noise(keys[2], (D, CONV_CH), D ** -0.5, 0.125, ((0, 8), (1, 4)))
    glu_proj = noise(keys[3], (D, CONV_CH), D ** -0.5, 0.125, ((0, 8), (1, 4)))
    recur_proj = noise(keys[4], (D, LRU_CH), D ** -0.5, 0.125, ((0, 8), (1, 4)))
    branch_proj = noise(keys[5], (D, LRU_CH), D ** -0.5, 0.125, ((0, 8), (1, 4)))
    channelwise_filter_taps = noise(keys[6], (KERNEL, CONV_CH), KERNEL ** -0.5, 1.0, ((1, 4),))
    group_gain = jnp.clip(1.0 + 0.18 * jax.random.normal(keys[7], (CONV_CH,), jnp.float32), 0.099609375, 1.8984375).astype(jnp.bfloat16)
    short_kernel = noise(keys[8], (SHORT, LRU_CH), SHORT ** -0.5, 3.0, ((1, 4),))
    decay_map = noise(keys[9], (LRU_HEADS, HEAD_CH, HEAD_CH), HEAD_CH ** -0.5, 0.75, ((0, 4),))
    entry_gate_matrix = noise(keys[10], (LRU_HEADS, HEAD_CH, HEAD_CH), HEAD_CH ** -0.5, 0.75, ((0, 4),))
    rate_param = draw_rate_param(jax.random.fold_in(keys[15], 71), 0)
    extra_decay = draw_extra_decay(jax.random.fold_in(keys[15], 71), 0)
    conv_out = noise(keys[13], (CONV_CH, D), (CONV_CH + LRU_CH) ** -0.5, 0.125, ((0, 4), (1, 8)))
    recur_out = noise(keys[14], (LRU_CH, D), (CONV_CH + LRU_CH) ** -0.5, 0.125, ((0, 4), (1, 8)))
    return dict(tokens=tokens, norm_gain=norm_gain, value_proj=value_proj, glu_proj=glu_proj, recur_proj=recur_proj, branch_proj=branch_proj, channelwise_filter_taps=channelwise_filter_taps, group_gain=group_gain, short_kernel=short_kernel, decay_map=decay_map, entry_gate_matrix=entry_gate_matrix, rate_param=rate_param, extra_decay=extra_decay, conv_out=conv_out, recur_out=recur_out)


eps = 1e-06
gate_scale = 8.0

def causal_taps(series, kernel):
    taps = kernel.shape[0]
    length = series.shape[0]
    padded = jnp.concatenate([jnp.zeros((taps - 1, series.shape[1]), jnp.float32), series], axis=0)
    total = jnp.zeros(series.shape, jnp.float32)
    for offset in range(taps):
        total = total + kernel[offset] * padded[offset:offset + length]
    return total

def merge_pair(earlier, later):
    return (earlier[0] * later[0], later[0] * earlier[1] + later[1])

def reference(tokens, norm_gain, value_proj, glu_proj, recur_proj, branch_proj, channelwise_filter_taps, group_gain, short_kernel, decay_map, entry_gate_matrix, rate_param, extra_decay, conv_out, recur_out):
    f32 = jnp.float32
    x_float = tokens.astype(f32)
    scale = lax.rsqrt(lax.optimization_barrier(jnp.mean(x_float * x_float, axis=-1, keepdims=True)) + eps)
    normed = (x_float * scale * norm_gain.astype(f32)).astype(jnp.bfloat16)
    value_part = jnp.dot(normed, value_proj, preferred_element_type=f32)
    glu_part = jnp.dot(normed, glu_proj, preferred_element_type=f32)
    arm_portion = jnp.dot(normed, branch_proj, preferred_element_type=f32)
    rec_input = jnp.dot(normed, recur_proj, preferred_element_type=f32).astype(jnp.bfloat16)
    gated = (value_part * jax.nn.sigmoid(glu_part)).astype(jnp.bfloat16)
    conv_sum = causal_taps(gated.astype(f32), channelwise_filter_taps.astype(f32))
    length = conv_sum.shape[0]
    grouped = conv_sum.reshape(length, CONV_CH // GROUP_CH, GROUP_CH)
    center = lax.optimization_barrier(jnp.mean(grouped, axis=-1, keepdims=True))
    spread = grouped - center
    var = lax.optimization_barrier(jnp.mean(spread * spread, axis=-1, keepdims=True))
    grouped = (spread * lax.rsqrt(var + eps)).reshape(length, CONV_CH)
    y_conv = jax.nn.silu(grouped * group_gain.astype(f32)).astype(jnp.bfloat16)
    rec_conv = causal_taps(rec_input.astype(f32), short_kernel.astype(f32)).astype(jnp.bfloat16)
    heads_view = rec_conv.astype(f32).reshape(length, LRU_HEADS, HEAD_CH)
    recur_gate = jax.nn.sigmoid(jnp.einsum('shi,hij->shj', heads_view, decay_map.astype(f32)).reshape(length, LRU_CH))
    input_gate = jax.nn.sigmoid(jnp.einsum('shi,hij->shj', heads_view, entry_gate_matrix.astype(f32)).reshape(length, LRU_CH))
    log_decay = -gate_scale * recur_gate * jax.nn.softplus(-rate_param)[None, :] + extra_decay
    decay = jnp.exp(log_decay)
    drive = jnp.sqrt(-jnp.expm1(2.0 * log_decay)) * input_gate * rec_conv.astype(f32)
    state = lax.associative_scan(merge_pair, (decay, drive), axis=0)[1]
    y_lru = (state * jax.nn.gelu(arm_portion, approximate=True)).astype(jnp.bfloat16)
    total = jnp.dot(y_conv, conv_out, preferred_element_type=f32) + jnp.dot(y_lru, recur_out, preferred_element_type=f32)
    return total.astype(jnp.bfloat16)
```

```python
import jax
import jax.numpy as jnp
from jax import lax
from jax.experimental import pallas as pl
from jax.experimental.pallas import tpu as pltpu
from jax.sharding import PartitionSpec as P

GROUP_CH = 64
HEAD_CH = 64
eps = 1e-06
gate_scale = 8.0
f32 = jnp.float32
bf16 = jnp.bfloat16


def grid_of(count):
    ny = 1
    while 2 * (2 * ny) * (2 * ny) <= count and count % (2 * ny) == 0:
        ny *= 2
    return count // ny, ny


def after(value, *others):
    return lax.optimization_barrier((value,) + others)[0]


def ring_gather(value, size, send):
    out = [None] * size
    out[0] = [value]
    if size == 2:
        out[1] = [send(value, 1)]
    if size <= 2:
        return out
    ahead = behind = value
    for step in range(1, (size - 1) // 2 + 1):
        ahead = send(ahead, 1)
        behind = send(behind, -1)
        out[size - step] = [ahead]
        out[step] = [behind]
    if size % 2 == 0:
        half = value.shape[0] // 2
        out[size // 2] = [send(ahead[:half], 1), send(behind[half:], -1)]
    return out


def norm_body(order_ref, x_ref, gain_ref, o_ref, *, parts):
    x = x_ref[...].astype(f32)
    scale = lax.rsqrt(jnp.mean(x * x, axis=-1, keepdims=True) + eps)
    width = x.shape[1] // parts
    for r in range(parts):
        if parts == 1:
            o_ref[...] = (x * scale * gain_ref[...].astype(f32)).astype(bf16)
        else:
            at = pl.ds(pl.multiple_of(order_ref[r] * width, 128), width)
            o_ref[:, r * width : (r + 1) * width] = (
                x_ref[:, at].astype(f32) * scale * gain_ref[:, at].astype(f32)
            ).astype(bf16)


def normalise(tokens, gain, order, parts):
    rows, width = tokens.shape
    aligned = (width // parts) % 128 == 0
    block = min(rows, 128)
    out = pl.pallas_call(
        lambda *refs: norm_body(*refs, parts=parts if aligned else 1),
        out_shape=jax.ShapeDtypeStruct((rows, width), bf16),
        grid_spec=pltpu.PrefetchScalarGridSpec(
            num_scalar_prefetch=1,
            grid=(rows // block,),
            in_specs=[
                pl.BlockSpec((block, width), lambda i, o: (i, 0)),
                pl.BlockSpec((1, width), lambda i, o: (0, 0)),
            ],
            out_specs=pl.BlockSpec((block, width), lambda i, o: (i, 0)),
        ),
        name="norm",
    )(order, tokens, gain)
    if not aligned:
        cut = out.reshape(rows, parts, width // parts)
        out = jnp.take(cut, order, axis=1).reshape(rows, width)
    return out


def project(x, weights):
    total = None
    at = 0
    for w in weights:
        part = jnp.dot(x[:, at : at + w.shape[0]], w[...], preferred_element_type=f32)
        total = part if total is None else total + part
        at += w.shape[0]
    return total


def expm1_neg(x):
    series = 1.0 + x * (1.0 / 8.0)
    for n in (7.0, 6.0, 5.0, 4.0, 3.0, 2.0):
        series = 1.0 + x * (1.0 / n) * series
    return jnp.where(x > -0.5, -x * series, 1.0 - jnp.exp(x))


def lru_body(*refs, count, rows):
    halo, x = refs[:2]
    weights = refs[2 : 2 + count]
    taps, decay_map, entry, soft, extra = refs[2 + count : 7 + count]
    state_ref, decay_ref, last_ref, prev, carry = refs[7 + count :]
    step = pl.program_id(0)
    width = taps.shape[1]

    @pl.when(step == 0)
    def _():
        head = project(halo[...], weights).astype(bf16).astype(f32)
        prev[...] = head[head.shape[0] - 8 :]
        carry[0:8] = jnp.ones((8, width), f32)
        carry[8:16] = jnp.zeros((8, width), f32)

    current = project(x[...], weights).astype(bf16).astype(f32)
    joined = jnp.concatenate([prev[...], current], axis=0)
    prev[...] = current[rows - 8 :]
    short = taps.shape[0]
    taps_f = taps[...].astype(f32)
    total = taps_f[short - 1 : short] * current
    for k in range(short - 1):
        at = 8 - short + 1 + k
        total = total + taps_f[k : k + 1] * joined[at : at + rows]
    conv = total.astype(bf16)
    recur_gate = jax.nn.sigmoid(jnp.dot(conv, decay_map[...], preferred_element_type=f32))
    input_gate = jax.nn.sigmoid(jnp.dot(conv, entry[...], preferred_element_type=f32))
    log_decay = -gate_scale * recur_gate * soft[...] + extra[...]
    a = jnp.exp(log_decay)
    b = jnp.sqrt(expm1_neg(2.0 * log_decay)) * input_gate * conv.astype(f32)
    a = a.reshape(rows // 8, 8, width)
    b = b.reshape(rows // 8, 8, width)
    place = lax.broadcasted_iota(jnp.int32, a.shape, 1)
    for shift in (1, 2, 4):
        a_before = pltpu.roll(a, shift, 1)
        b_before = pltpu.roll(b, shift, 1)
        inside = place >= shift
        b = jnp.where(inside, a * b_before + b, b)
        a = jnp.where(inside, a * a_before, a)
    decay, state = carry[0:1], carry[8:9]
    for g in range(rows // 8):
        now_state = a[g] * state + b[g]
        now_decay = a[g] * decay
        state_ref[8 * g : 8 * g + 8] = now_state
        decay_ref[8 * g : 8 * g + 8] = now_decay
        state, decay = now_state[7:8], now_decay[7:8]
    carry[0:8] = jnp.broadcast_to(decay, (8, width))
    carry[8:16] = jnp.broadcast_to(state, (8, width))
    last_ref[0:8] = jnp.broadcast_to(decay, (8, width))
    last_ref[8:16] = jnp.broadcast_to(state, (8, width))


def whole(array):
    return pl.BlockSpec(array.shape, lambda i, *_: (0,) * array.ndim)


def lru_local(halo, x, weights, taps, decay_map, entry, soft, extra):
    rows, width = extra.shape
    block = min(rows, 128)
    row = lambda cols: pl.BlockSpec((block, cols), lambda i: (i, 0))
    return pl.pallas_call(
        lambda *refs: lru_body(*refs, count=len(weights), rows=block),
        out_shape=(
            jax.ShapeDtypeStruct((rows, width), f32),
            jax.ShapeDtypeStruct((rows, width), f32),
            jax.ShapeDtypeStruct((16, width), f32),
        ),
        grid=(rows // block,),
        in_specs=[whole(halo), row(x.shape[1])]
        + [whole(w) for w in weights]
        + [whole(taps), whole(decay_map), whole(entry), whole(soft), row(width)],
        out_specs=(row(width), row(width), pl.BlockSpec((16, width), lambda i: (0, 0))),
        scratch_shapes=[pltpu.VMEM((8, width), f32), pltpu.VMEM((16, width), f32)],
        name="lru",
    )(halo, x, *weights, taps, decay_map, entry, soft, extra)


def group_mean(x, average):
    high = x.astype(bf16)
    rest = x - high.astype(f32)
    low = rest.astype(bf16)
    lower = (rest - low.astype(f32)).astype(bf16)
    dot = lambda v: jnp.dot(v, average, preferred_element_type=f32)
    return dot(high) + (dot(low) + dot(lower))


def conv_body(*refs, count, rows, back):
    halo, x = refs[:2]
    weights = refs[2 : 2 + count]
    taps, gain, average = refs[2 + count : 5 + count]
    out_ref, gate_ref, window = refs[5 + count :]
    step = pl.program_id(0)
    wide, width = taps.shape

    def split(acc):
        gated = acc[:, width : 2 * width] * jax.nn.sigmoid(acc[:, 2 * width :])
        return acc[:, :width], gated.astype(bf16).astype(f32)

    @pl.when(step == 0)
    def _():
        window[0:back] = split(project(halo[...], weights))[1]

    arm, gated = split(project(x[...], weights))
    gate_ref[...] = jax.nn.gelu(arm, approximate=True)
    window[back : back + rows] = gated
    taps_f = taps[...].astype(f32)
    first = back - (wide - 1)
    total = None
    for residue in range(8):
        part = None
        for k in range(wide):
            if (first + k) % 8 != residue:
                continue
            at = first + k - residue
            extent = rows + 8 if residue else rows
            term = taps_f[k : k + 1] * window[at : at + extent]
            part = term if part is None else part + term
        if part is not None:
            part = part[residue : residue + rows]
            total = part if total is None else total + part
    window[0:back] = gated[rows - back :]
    spread = total - group_mean(total, average[...])
    var = group_mean(spread * spread, average[...])
    y = spread * lax.rsqrt(var + eps) * gain[...].astype(f32)
    out_ref[...] = (y * jax.nn.sigmoid(y)).astype(bf16)


def conv_local(halo, x, weights, taps, gain, average):
    rows, width = x.shape[0], taps.shape[1]
    block = min(rows, 128)
    back = halo.shape[0]
    row = lambda cols: pl.BlockSpec((block, cols), lambda i: (i, 0))
    return pl.pallas_call(
        lambda *refs: conv_body(*refs, count=len(weights), rows=block, back=back),
        out_shape=(
            jax.ShapeDtypeStruct((rows, width), bf16),
            jax.ShapeDtypeStruct((rows, width), f32),
        ),
        grid=(rows // block,),
        in_specs=[whole(halo), row(x.shape[1])]
        + [whole(w) for w in weights]
        + [whole(taps), whole(gain), whole(average)],
        out_specs=(row(width), row(width)),
        scratch_shapes=[pltpu.VMEM((back + block + 8, width), f32)],
        name="conv",
    )(halo, x, *weights, taps, gain, average)


def out_body(*refs, count, aligned):
    order, _ = refs[:2]
    y_conv, state, decay, gate, incoming = refs[2:7]
    weights = refs[7 : 7 + count]
    out = refs[7 + count]
    y_lru = ((state[...] + decay[...] * incoming[...]) * gate[...]).astype(bf16)
    y = jnp.concatenate([y_conv[...], y_lru], axis=1)
    for r, w in enumerate(weights):
        width = w.shape[1]
        part = jnp.dot(y, w[...], preferred_element_type=f32).astype(out.dtype)
        if aligned:
            out[:, pl.ds(pl.multiple_of(order[r] * width, 128), width)] = part
        else:
            out[:, r * width : (r + 1) * width] = part


def out_rows(which, order, y_conv, state, decay, gate, incoming, weights, rows, dtype):
    width = y_conv.shape[1]
    cols = sum(w.shape[1] for w in weights)
    block = min(rows, 128)
    row = pl.BlockSpec((block, width), lambda i, o, b: (b[0] * (rows // block) + i, 0))
    aligned = weights[0].shape[1] % 128 == 0
    return pl.pallas_call(
        lambda *refs: out_body(*refs, count=len(weights), aligned=aligned),
        out_shape=jax.ShapeDtypeStruct((rows, cols), dtype),
        grid_spec=pltpu.PrefetchScalarGridSpec(
            num_scalar_prefetch=2,
            grid=(rows // block,),
            in_specs=[row, row, row, row, whole(incoming)] + [whole(w) for w in weights],
            out_specs=pl.BlockSpec((block, cols), lambda i, o, b: (i, 0)),
        ),
        name="out",
    )(order, which, y_conv, state, decay, gate, incoming, *weights)


def block_diagonal(blocks):
    heads, size, _ = blocks.shape
    eye = jnp.eye(heads, dtype=blocks.dtype)
    return (eye[:, None, :, None] * blocks[:, :, None, :]).reshape(heads * size, heads * size)


def body(
    tokens,
    norm_gain,
    value_proj,
    glu_proj,
    recur_proj,
    branch_proj,
    channelwise_filter_taps,
    group_gain,
    short_kernel,
    decay_map,
    entry_gate_matrix,
    rate_param,
    extra_decay,
    conv_out,
    recur_out,
):
    local_rows, model = tokens.shape
    width = value_proj.shape[1]
    sp = lax.axis_size("sp")
    tp = lax.axis_size("tp")
    nz, ny = grid_of(sp)
    place = lax.axis_index("sp")
    spot = lax.axis_index("tp")
    z, y = place // ny, place % ny

    def send_z(value, step):
        pairs = [(a * ny + b, ((a + step) % nz) * ny + b) for a in range(nz) for b in range(ny)]
        return lax.ppermute(value, "sp", pairs)

    def send_y(value, step):
        pairs = [(a * ny + b, a * ny + (b + step) % ny) for a in range(nz) for b in range(ny)]
        return lax.ppermute(value, "sp", pairs)

    flat = lambda groups: [piece for group in groups for piece in group]
    order = jnp.stack(
        [((z + dz) % nz) * ny + (y + dy) % ny for dz in range(nz) for dy in range(ny)]
    ).astype(jnp.int32)

    def rows_of(shard):
        stack = jnp.concatenate(flat(ring_gather(shard, ny, send_y)), axis=0)
        return flat(ring_gather(stack, nz, send_z))

    recur_w = rows_of(recur_proj)
    mixed_w = rows_of(jnp.concatenate([branch_proj, value_proj, glu_proj], axis=1))
    out_w = []
    for group in ring_gather(jnp.concatenate([conv_out, recur_out], axis=0), nz, send_z):
        joined = group[0] if len(group) == 1 else jnp.concatenate(group, axis=0)
        for piece in ring_gather(joined, ny, send_y):
            out_w.append(piece[0] if len(piece) == 1 else jnp.concatenate(piece, axis=0))

    back = 32
    halo = lax.ppermute(tokens[local_rows - back :], "sp", [(i, i + 1) for i in range(sp - 1)])
    gain = norm_gain[None, :]
    normed = normalise(tokens, gain, order, sp)
    normed_halo = normalise(halo, gain, order, sp)

    soft = jax.nn.softplus(-rate_param)[None, :]
    running_state, running_decay, last = lru_local(
        normed_halo,
        normed,
        recur_w,
        short_kernel,
        block_diagonal(decay_map),
        block_diagonal(entry_gate_matrix),
        soft,
        extra_decay,
    )
    ends = jnp.stack([last[0], last[8]])
    ends = lax.all_to_all(jnp.broadcast_to(ends[None], (sp,) + ends.shape), "sp", 0, 0)
    incoming = jnp.zeros((width,), f32)
    for hop in range(sp - 1):
        incoming = jnp.where(hop < place, ends[hop, 0] * incoming + ends[hop, 1], incoming)

    average = block_diagonal(jnp.full((width // GROUP_CH, GROUP_CH, GROUP_CH), 1.0 / GROUP_CH, bf16))
    y_conv, gate = conv_local(
        normed_halo, normed, mixed_w, channelwise_filter_taps, group_gain[None, :], average
    )

    core, column, columns = spot % 2, spot // 2, tp // 2
    rows = local_rows // tp

    def partial(col, which_core, dtype):
        which = (col * 2 + which_core).astype(jnp.int32)[None]
        return out_rows(
            which, order, y_conv, running_state, running_decay, gate, incoming[None, :], out_w, rows, dtype
        )

    swap = [(i, i ^ 1) for i in range(tp)]
    total = None
    for step in list(range(1, columns)) + [0]:
        target = (column + step) % columns
        other = lax.ppermute(partial(target, 1 - core, bf16), "tp", swap)
        mine = partial(target, core, f32) + other.astype(f32)
        if step:
            pairs = [(i, ((i // 2 + step) % columns) * 2 + i % 2) for i in range(tp)]
            mine = lax.ppermute(mine.astype(bf16), "tp", pairs).astype(f32)
        total = mine if total is None else total + mine
    mixed = total.astype(bf16)
    if (model // sp) % 128:
        cut = mixed.reshape(rows, sp, model // sp)
        mixed = jnp.take(cut, jnp.argsort(order), axis=1).reshape(rows, model)
    return mixed


def solution(mesh):
    in_specs = (
        P("sp", None),
        P(),
        P("sp", "tp"),
        P("sp", "tp"),
        P("sp", "tp"),
        P("sp", "tp"),
        P(None, "tp"),
        P("tp"),
        P(None, "tp"),
        P("tp", None, None),
        P("tp", None, None),
        P("tp"),
        P("sp", "tp"),
        P("tp", "sp"),
        P("tp", "sp"),
    )
    out_specs = P(("sp", "tp"), None)
    return jax.shard_map(body, mesh=mesh, in_specs=in_specs, out_specs=out_specs, check_vma=False)
```
